32 devices in a mesh: grp: 2 (over x), ep: 16 (over z, y, core).
Axes of the slice: x: 2, y: 2, z: 4, core: 2. Of those that a mesh axis runs over, the one named last changes fastest.
Arguments:
- tokens: bfloat16 [1024, 2048], P(('grp', 'ep')), parts along dimension 0, may hold values from -6 to 6
- routes: int32 [1024, 8], P(('grp', 'ep')), parts along dimension 0, may hold values from 0 to 15, all different within a row; in each aligned block of 32 rows (0 to 31, 32 to 63, ...) at most 24 rows name the same one
- gates: float32 [1024, 8], P(('grp', 'ep')), parts along dimension 0, may hold values from 0.1 to 0.6
- norm_gain: float32 [2048], replicated, may hold values from 0.1 to 1.9
- expert_gate: bfloat16 [16, 2048, 512], P('ep'), may hold values from -0.125 to 0.125
- expert_up: bfloat16 [16, 2048, 512], P('ep'), may hold values from -0.125 to 0.125
- expert_down: bfloat16 [16, 512, 2048], P('ep'), may hold values from -0.25 to 0.25
- shared_gate: bfloat16 [2048, 512], replicated, may hold values from -0.125 to 0.125
- shared_up: bfloat16 [2048, 512], replicated, may hold values from -0.125 to 0.125
- shared_down: bfloat16 [512, 2048], replicated, may hold values from -0.25 to 0.25
Outputs:
- mixed: bfloat16 [1024, 2048], P(('grp', 'ep')), parts along dimension 0
The draws below stay inside these ranges and needn't reach their ends.
There are 2 independent parts, one for each index of `grp`. The reference program is written for one: setup_inputs(seed, part) draws one part's arguments, and reference() takes and returns one part's arrays. A program takes and returns all parts, laid end to end along the dimension named above; an argument that names none is the same for every part. Nothing has to cross between parts.
Inputs may be any that keep to these rules, and one draw needn't show every extreme that they name: `routes`: each row names 8 different experts; among the rows of one device no expert is named by more than 24 rows, a bound that some block reaches.
All inputs are finite; a program needn't handle non-finite values.
Results may differ from the reference program's by a relative error of at most 0.013.
Values may be sent and summed in bfloat16 or wider, within the bound.
No kernel may reach another device: no remote copies, remote signals or barrier semaphores. Data moves between devices by JAX's collectives and lax.ppermute only.
A program may use at most 128 MiB of HBM per device.

```python
import math
import jax
import jax.numpy as jnp
import numpy as np
from jax import lax

D = 2048
DE = 512
TOPK = 8
TOK_DEV = 32
CAP = 24
EXPERTS = 16
TOKENS = 512


def shard_levels(stream_key, shape, cuts, smallest, top_value):
    def one(dim, shards_of):
        draws = jax.random.uniform(jax.random.fold_in(jax.random.fold_in(stream_key, 6), dim), (shards_of,), jnp.float32, smallest / len(cuts), top_value / len(cuts))
        return jnp.repeat(jnp.exp(draws), shape[dim] // shards_of).reshape((-1,) + (1,) * (len(shape) - dim - 1))

    loudness = one(*cuts[0])
    for cut in cuts[1:]:
        loudness = loudness * one(*cut)
    return loudness


def assign_block(stream_key, own, number, rows, number_of, top, bound, lean):
    sequence = jax.random.permutation(stream_key, number_of)
    crowded, ordinary = shares(number_of, rows * top, bound, lean, True), shares(number_of, rows * top, bound, lean, False)
    places = jnp.arange(number_of)

    def named(tallies, offset_by):
        used = int((tallies > 0).sum())
        fixed = max(1, used // 4)
        moved = fixed + (places - fixed + offset_by * (used - fixed)) % max(1, number_of - fixed)
        return jnp.zeros((number_of,), jnp.int32).at[sequence[jnp.where(places < fixed, places, moved)]].set(jnp.asarray(tallies, jnp.int32))

    tallies = jnp.where(number % 4 == 0, named(crowded, number // 4), named(ordinary, number - number // 4 - 1))
    mixed = jax.random.permutation(jax.random.fold_in(own, 3), number_of)
    donor, taker = mixed[0:number_of // 2 * 2:2], mixed[1:number_of // 2 * 2:2]
    slack = jnp.minimum(tallies[donor] - 1, bound - tallies[taker]) // 2
    slack = jnp.where((donor == sequence[0]) | (taker == sequence[0]) | (tallies[taker] == 0), 0, jnp.maximum(slack, 0))
    moved = jax.random.randint(jax.random.fold_in(own, 4), (number_of // 2,), 0, 1 << 20) % (slack + 1)
    tallies = tallies.at[donor].add(-moved).at[taker].add(moved)
    items = jnp.searchsorted(jnp.cumsum(tallies), jnp.arange(rows * top), side="right").astype(jnp.int32)
    listing = items.reshape(top, rows).T
    listing = listing[jax.random.permutation(jax.random.fold_in(own, 1), rows)]
    offset_by = jax.random.randint(jax.random.fold_in(own, 2), (rows, 1), 0, top)
    return jnp.take_along_axis(listing, (jnp.arange(top)[None, :] + offset_by) % top, axis=1)


def shares(count, total, bound, skew, full):
    weights = [(1 << 20) // math.isqrt(rank ** skew) + 1 for rank in range(1, count + 1)]
    largest = bound if full else min(bound, max(-(-total // count), total * weights[0] // sum(weights)))
    least = 1 if total - largest >= count - 1 else 0
    holding, rest = [largest] + [least] * (count - 1), total - largest - least * (count - 1)
    while rest > 0:
        movable = [i for i in range(1, count) if holding[i] < largest] or [i for i in range(1, count) if holding[i] < bound]
        pool, remaining = sum([weights[i] for i in movable]), rest
        for i in movable:
            extra = min(bound - holding[i], max(1, remaining * weights[i] // pool), rest)
            holding[i] = holding[i] + extra
            rest = rest - extra
    return np.array(holding)


def normal_values(own_key, extent, spread, bound, pieces=(), kind=jnp.bfloat16):
    entries = spread * jax.random.normal(own_key, extent, jnp.float32)
    if pieces:
        entries = entries * shard_levels(own_key, extent, pieces, -0.22, 0.18)
    return jnp.clip(entries, -bound, bound).astype(kind)


def setup_inputs(seed: int = 0, part: int = 0) -> dict:
    arg_keys = jax.random.split(jax.random.key(seed), 11)
    own_keys = jax.random.split(jax.random.fold_in(arg_keys[10], part), 11)
    tokens = normal_values(own_keys[0], (TOKENS, D), 1.0, 6.0, ((0, 16),))
    routes_keys = jax.random.split(jax.random.fold_in(own_keys[1], 1), TOKENS // TOK_DEV)
    routes_turns = jax.random.permutation(jax.random.fold_in(own_keys[1], 3), TOKENS // TOK_DEV)
    routes = jax.vmap(lambda own, number: assign_block(jax.random.fold_in(own_keys[1], 2), own, number, TOK_DEV, EXPERTS, TOPK, CAP, 2))(routes_keys, routes_turns).reshape((TOKENS, TOPK))
    gates = jnp.clip(0.1 + 0.5 * jax.random.uniform(own_keys[2], (TOKENS, TOPK), jnp.float32) ** shard_levels(own_keys[2], (TOKENS, TOPK), ((0, 16),), -0.2, 0.2), 0.1, 0.6)
    norm_gain = jnp.clip(1.0 + 0.18 * jax.random.normal(arg_keys[3], (D,), jnp.float32), 0.1, 1.9)
    expert_gate = normal_values(arg_keys[4], (EXPERTS, D, DE), D ** -0.5, 0.125, ((0, 16),))
    expert_up = normal_values(arg_keys[5], (EXPERTS, D, DE), D ** -0.5, 0.125, ((0, 16),))
    expert_down = normal_values(arg_keys[6], (EXPERTS, DE, D), DE ** -0.5, 0.25, ((0, 16),))
    shared_gate = normal_values(arg_keys[7], (D, DE), D ** -0.5, 0.125)
    shared_up = normal_values(arg_keys[8], (D, DE), D ** -0.5, 0.125)
    shared_down = normal_values(arg_keys[9], (DE, D), DE ** -0.5, 0.25)
    return {"tokens": tokens, "routes": routes, "gates": gates, "norm_gain": norm_gain, "expert_gate": expert_gate, "expert_up": expert_up, "expert_down": expert_down, "shared_gate": shared_gate, "shared_up": shared_up, "shared_down": shared_down}


def norm_rows(tokens, norm_gain):
    values = tokens.astype(jnp.float32)
    scale = lax.rsqrt(lax.optimization_barrier(jnp.mean(values * values, axis=-1, keepdims=True)) + 1e-06)
    return (values * scale * norm_gain).astype(jnp.bfloat16)

def expert_rows(in_rows, w_gate, w_up, w_down):
    gate_pre = jnp.dot(in_rows, w_gate, preferred_element_type=jnp.float32)
    up_pre = jnp.dot(in_rows, w_up, preferred_element_type=jnp.float32)
    hidden = (jax.nn.silu(gate_pre) * up_pre).astype(jnp.bfloat16)
    return jnp.dot(hidden, w_down, preferred_element_type=jnp.float32).astype(jnp.bfloat16)

def reference(tokens, routes, gates, norm_gain, expert_gate, expert_up, expert_down, shared_gate, shared_up, shared_down):
    normed = norm_rows(tokens, norm_gain)
    chosen = lax.optimization_barrier(jnp.sum(jax.nn.one_hot(routes, EXPERTS, dtype=jnp.float32) * gates[:, :, None], axis=1))

    def one_expert(carry, packed):
        w_gate, w_up, w_down, weight = packed
        answer = expert_rows(normed, w_gate, w_up, w_down)
        return (carry + weight[:, None] * answer.astype(jnp.float32), None)
    start = jnp.zeros((normed.shape[0], normed.shape[1]), jnp.float32)
    routed, _ = lax.scan(one_expert, start, (expert_gate, expert_up, expert_down, chosen.T))
    gate_pre = jnp.dot(normed, shared_gate, preferred_element_type=jnp.float32)
    up_pre = jnp.dot(normed, shared_up, preferred_element_type=jnp.float32)
    shared_hidden = (jax.nn.silu(gate_pre) * up_pre).astype(jnp.bfloat16)
    shared = jnp.dot(shared_hidden, shared_down, preferred_element_type=jnp.float32)
    return (routed + shared).astype(jnp.bfloat16)
```

```python
import jax
import jax.numpy as jnp
from jax import lax
from jax.sharding import PartitionSpec as P


def norm_rows(tokens, norm_gain):
    values = tokens.astype(jnp.float32)
    scale = lax.rsqrt(jnp.mean(values * values, axis=-1, keepdims=True) + 1e-06)
    return (values * scale * norm_gain).astype(jnp.bfloat16)


def ffn(in_rows, w_gate, w_up, w_down):
    gate_pre = jnp.dot(in_rows, w_gate, preferred_element_type=jnp.float32)
    up_pre = jnp.dot(in_rows, w_up, preferred_element_type=jnp.float32)
    hidden = (jax.nn.silu(gate_pre) * up_pre).astype(jnp.bfloat16)
    return jnp.dot(hidden, w_down, preferred_element_type=jnp.float32)


def split3(x):
    a = lax.reduce_precision(x, 8, 7)
    b = lax.reduce_precision(x - a, 8, 7)
    c = x - a - b
    return [v.astype(jnp.bfloat16) for v in (a, b, c)]


def local(
    tokens, routes, gates, norm_gain,
    expert_gate, expert_up, expert_down,
    shared_gate, shared_up, shared_down,
):
    width = tokens.shape[1]
    groups = lax.axis_size("ep")
    me = lax.axis_index("ep")
    normed = norm_rows(tokens, norm_gain)
    naming = routes[:, :, None] == jnp.arange(groups, dtype=jnp.int32)[None, None, :]
    weights = jnp.sum(jnp.where(naming, gates[:, :, None], 0.0), axis=1)
    cols = jnp.concatenate(split3(weights), axis=1)
    pad = -cols.shape[1] % 128
    cols = jnp.pad(cols, ((0, 0), (0, pad)))
    sent = jnp.concatenate([normed, cols], axis=1)
    every = lax.all_gather(sent, "ep", axis=0, tiled=True)
    shared = ffn(normed, shared_gate, shared_up, shared_down)
    flat = every[:, :width]
    lane = jnp.arange(groups * 3, dtype=jnp.int32) % groups
    extra = every[:, width : width + 3 * groups].astype(jnp.float32)
    mine = jnp.sum(jnp.where(lane[None, :] == me, extra, 0.0), axis=1, keepdims=True)
    answers = ffn(flat, expert_gate[0], expert_up[0], expert_down[0])
    partial = (mine * answers.astype(jnp.bfloat16).astype(jnp.float32)).astype(jnp.bfloat16)
    routed = lax.psum_scatter(partial, "ep", scatter_dimension=0, tiled=True)
    return (routed.astype(jnp.float32) + shared).astype(jnp.bfloat16)


def solution(mesh):
    return jax.shard_map(
        local,
        mesh=mesh,
        in_specs=(
            P(("grp", "ep"), None),
            P(("grp", "ep"), None),
            P(("grp", "ep"), None),
            P(),
            P("ep", None, None),
            P("ep", None, None),
            P("ep", None, None),
            P(),
            P(),
            P(),
        ),
        out_specs=P(("grp", "ep"), None),
        check_vma=False,
    )
```

```python
import jax
import jax.numpy as jnp
from jax import lax
from jax.experimental import pallas as pl
from jax.experimental.pallas import tpu as pltpu
from jax.sharding import PartitionSpec as P

LANES = 128


def ffn(in_rows, w_gate, w_up, w_down):
    gate_pre = jnp.dot(in_rows, w_gate, preferred_element_type=jnp.float32)
    up_pre = jnp.dot(in_rows, w_up, preferred_element_type=jnp.float32)
    hidden = (jax.nn.silu(gate_pre) * up_pre).astype(jnp.bfloat16)
    return jnp.dot(hidden, w_down, preferred_element_type=jnp.float32)


def prologue(tokens, routes, gates, norm_gain, groups):
    rows, width = tokens.shape
    extra = -(-3 * groups // LANES) * LANES

    def body(tok_ref, route_ref, gate_ref, gain_ref, out_ref):
        values = tok_ref[...].astype(jnp.float32)
        scale = lax.rsqrt(jnp.mean(values * values, axis=-1, keepdims=True) + 1e-06)
        out_ref[:, :width] = (values * scale * gain_ref[...]).astype(jnp.bfloat16)
        line = lax.broadcasted_iota(jnp.int32, (extra, rows), 0)
        expert = line % groups
        term = line // groups
        weight = jnp.zeros((extra, rows), jnp.float32)
        for k in range(routes.shape[1]):
            weight += jnp.where(route_ref[k : k + 1, :] == expert, gate_ref[k : k + 1, :], 0.0)
        first = weight.astype(jnp.bfloat16).astype(jnp.float32)
        second = (weight - first).astype(jnp.bfloat16).astype(jnp.float32)
        third = weight - first - second
        cols = jnp.where(term == 0, first, jnp.where(term == 1, second, jnp.where(term == 2, third, 0.0)))
        square = (extra, extra)
        same = lax.broadcasted_iota(jnp.int32, square, 0) == lax.broadcasted_iota(jnp.int32, square, 1)
        turned = lax.dot_general(
            cols.astype(jnp.bfloat16),
            same.astype(jnp.float32).astype(jnp.bfloat16),
            (((0,), (0,)), ((), ())),
            preferred_element_type=jnp.float32,
        )
        out_ref[:, width:] = turned.astype(jnp.bfloat16)

    return pl.pallas_call(
        body, out_shape=jax.ShapeDtypeStruct((rows, width + extra), jnp.bfloat16), name="prologue"
    )(tokens, routes.T, gates.T, norm_gain.reshape(1, width))


def experts(pieces, after, mask, w_gate, w_up, w_down, cuts):
    count = sum(p.shape[0] for p in pieces)
    _, width, hidden = w_gate.shape
    quarter = count // 4
    rows = pieces[0].shape[0]
    planes = quarter // rows
    whole = pieces[0].shape[1]
    deep = width // cuts
    tall = hidden // 2

    def body(*refs):
        ins = refs[: len(pieces)]
        rest = refs[len(pieces) + len(after) :]
        mask_ref, g_hbm, u_hbm, d_hbm, own_ref = rest[:5]
        near_refs = rest[5 : 5 + planes]
        far_ref, x_ref, g_ref, u_ref, d_ref, sems = rest[5 + planes :]
        loads = []
        for i, ref in enumerate(ins):
            place = x_ref.at[pl.ds(i * rows, rows)]
            loads.append(pltpu.make_async_copy(ref, place, sems.at[2 * cuts + 2 + i]))
            loads[-1].start()
        copies = []
        for c in range(cuts):
            span = pl.ds(c * deep, deep)
            copies.append(
                (
                    pltpu.make_async_copy(g_hbm.at[0, span], g_ref.at[span], sems.at[2 * c]),
                    pltpu.make_async_copy(u_hbm.at[0, span], u_ref.at[span], sems.at[2 * c + 1]),
                )
            )
        downs = []
        for c in range(2):
            span = pl.ds(c * tall, tall)
            downs.append(pltpu.make_async_copy(d_hbm.at[0, span], d_ref.at[span], sems.at[2 * cuts + c]))
        for pair in copies:
            pair[0].start()
            pair[1].start()
        for one in downs:
            one.start()
        for one in loads:
            one.wait()
        terms = x_ref[:, width:].astype(jnp.float32) * mask_ref[...]
        weight = jnp.sum(terms, axis=1, keepdims=True)
        gate_pre = jnp.zeros((count, hidden), jnp.float32)
        up_pre = jnp.zeros((count, hidden), jnp.float32)
        for c, pair in enumerate(copies):
            span = slice(c * deep, (c + 1) * deep)
            x = x_ref[:, span]
            pair[0].wait()
            gate_pre += jnp.dot(x, g_ref[span, :], preferred_element_type=jnp.float32)
            pair[1].wait()
            up_pre += jnp.dot(x, u_ref[span, :], preferred_element_type=jnp.float32)
        act = (jax.nn.silu(gate_pre) * up_pre).astype(jnp.bfloat16)
        downs[0].wait()
        downs[1].wait()
        out = jnp.dot(act, d_ref[...], preferred_element_type=jnp.float32)
        out = (out * weight).astype(jnp.bfloat16)
        own_ref[...] = out[:quarter]
        for i, ref in enumerate(near_refs):
            ref[...] = out[quarter + i * rows : quarter + (i + 1) * rows]
        far_ref[...] = out[2 * quarter :]

    hbm = pl.BlockSpec(memory_space=pl.ANY)
    outs = [(quarter, width)] + [(rows, width)] * planes + [(2 * quarter, width)]
    return pl.pallas_call(
        body,
        in_specs=[hbm] * (len(pieces) + len(after)) + [pl.BlockSpec(mask.shape, lambda: (0, 0))] + [hbm] * 3,
        out_specs=[pl.BlockSpec(s, lambda: (0, 0)) for s in outs],
        out_shape=[jax.ShapeDtypeStruct(s, jnp.bfloat16) for s in outs],
        scratch_shapes=[
            pltpu.VMEM((count, whole), jnp.bfloat16),
            pltpu.VMEM((width, hidden), jnp.bfloat16),
            pltpu.VMEM((width, hidden), jnp.bfloat16),
            pltpu.VMEM((hidden, width), jnp.bfloat16),
            pltpu.SemaphoreType.DMA((2 * cuts + 2 + len(pieces),)),
        ],
        name="experts",
    )(*pieces, *after, mask, w_gate, w_up, w_down)


def local(
    tokens, routes, gates, norm_gain,
    expert_gate, expert_up, expert_down,
    shared_gate, shared_up, shared_down,
):
    rows, width = tokens.shape
    groups = lax.axis_size("ep")
    me = lax.axis_index("ep")
    sent = prologue(tokens, routes, gates, norm_gain, groups)
    lane = jnp.arange(sent.shape[1] - width, dtype=jnp.int32)
    mask = ((lane % groups == me) & (lane < 3 * groups)).astype(jnp.float32)[None, :]

    def swap(x, bits):
        return lax.ppermute(x, "ep", [(i, i ^ bits) for i in range(groups)])

    planes = groups // 4
    batches = [list(range(planes))]
    pieces = {}
    arrived = {k: swap(sent, 4 * k) if k else sent for batch in batches for k in batch}
    for k, mine in arrived.items():
        near = swap(mine, 2)
        pieces[k] = [mine, near, swap(mine, 1), swap(near, 1)]
    total = ffn(sent[:, :width], shared_gate, shared_up, shared_down)
    after = []
    for batch in batches:
        ordered = [pieces[k][i] for i in range(4) for k in batch]
        own, *nears, far = experts(ordered, after, mask, expert_gate, expert_up, expert_down, 4)
        back = swap(far, 1).astype(jnp.float32)
        half = len(batch) * rows
        after = []
        for i, k in enumerate(batch):
            span = slice(i * rows, (i + 1) * rows)
            near = (nears[i].astype(jnp.float32) + back[half:][span]).astype(jnp.bfloat16)
            after.append(near)
            one = own[span].astype(jnp.float32) + back[:half][span] + swap(near, 2).astype(jnp.float32)
            if k:
                one = swap(one.astype(jnp.bfloat16), 4 * k).astype(jnp.float32)
            total = total + one
    return total.astype(jnp.bfloat16)


def solution(mesh):
    return jax.shard_map(
        local,
        mesh=mesh,
        in_specs=(
            P(("grp", "ep"), None),
            P(("grp", "ep"), None),
            P(("grp", "ep"), None),
            P(),
            P("ep", None, None),
            P("ep", None, None),
            P("ep", None, None),
            P(),
            P(),
            P(),
        ),
        out_specs=P(("grp", "ep"), None),
        check_vma=False,
    )
```
